32 devices in a mesh: grp: 2 (over y), sp: 4 (over z), tp: 4 (over x, core).
Axes of the slice: x: 2, y: 2, z: 4, core: 2. Of those that a mesh axis runs over, the one named last changes fastest.
Arguments:
- latent: bfloat16 [4096, 4096], P(('grp', 'sp', 'tp')), parts along dimension 0, may hold values from -260 to 260
- context: bfloat16 [1536, 4096], P(('grp', 'sp')), parts along dimension 0, may hold values from -6 to 6
- conditioning: bfloat16 [8192], P(('grp', 'sp')), parts along dimension 0, may hold values from -6 to 6
- norm_gain: float32 [4096], replicated, may hold values from 0.1 to 1.9
- shift_weight: bfloat16 [4096, 4096], P('sp', 'tp'), may hold values from -0.09375 to 0.09375
- scale_weight: bfloat16 [4096, 4096], P('sp', 'tp'), may hold values from -0.09375 to 0.09375
- gate_weight: bfloat16 [4096, 4096], P('sp', 'tp'), may hold values from -0.09375 to 0.09375
- query_weight: bfloat16 [4096, 1024], P(None, 'tp'), may hold values from -3 to 3
- key_weight: bfloat16 [4096, 512], P(None, 'tp'), may hold values from -3 to 3
- value_weight: bfloat16 [4096, 512], P(None, 'tp'), may hold values from -0.09375 to 0.09375
- out_weight: bfloat16 [1024, 4096], P(None, 'tp'), may hold values from -1.5 to 1.5
- sink_logit: float32 [16], P('tp'), may hold values from 3 to 7
Outputs:
- mixed: bfloat16 [4096, 4096], P(('grp', 'sp', 'tp')), parts along dimension 0
The draws below stay inside these ranges and needn't reach their ends.
There are 2 independent parts, one for each index of `grp`. The reference program is written for one: setup_inputs(seed, part) draws one part's arguments, and reference() takes and returns one part's arrays. A program takes and returns all parts, laid end to end along the dimension named above; an argument that names none is the same for every part. Nothing has to cross between parts.
All inputs are finite; a program needn't handle non-finite values.
Results may differ from the reference program's by a relative error of at most 0.012.
The reference program's roundings to bfloat16 on the way count: a program that leaves them out, or rounds other values in their place, can miss the bound.
Values may be sent and summed in bfloat16 or wider, within the bound.
A program may use at most 64 MiB of HBM per device.

```python
import math
import jax
import jax.numpy as jnp
from jax import lax

D = 4096
HEADS = 16
KV_HEADS = 8
HD = 64
GRID_W = 64
WIN = 128
CTX = 768
SEQ = 2048


def paired_projections(seed_key):
    query_rows = jax.random.truncated_normal(jax.random.fold_in(seed_key, 11), -4.0, 4.0, (D, HEADS * HD), jnp.float32) / math.sqrt(D)
    key_rows = jax.random.truncated_normal(jax.random.fold_in(seed_key, 12), -4.0, 4.0, (D, KV_HEADS * HD), jnp.float32) / math.sqrt(D)
    return (query_rows, key_rows)


def draw_query_weight(key, part):
    return paired_projections(key)[0].astype(jnp.bfloat16)


def draw_key_weight(key, part):
    return paired_projections(key)[1].astype(jnp.bfloat16)


def draw_latent(key, part):
    values_drawn = jax.random.truncated_normal(jax.random.fold_in(key, 1), -6.0, 6.0, (SEQ, D), jnp.float32)
    return values_drawn.astype(jnp.bfloat16)


def block_scale(rng, extent, cuts, least, high):
    factor_of, own = 1.0, jax.random.fold_in(rng, 6)
    for dim, blocks in cuts:
        draws = jnp.exp(jax.random.uniform(jax.random.fold_in(own, dim), (blocks,), jnp.float32, least / len(cuts), high / len(cuts)))
        factor_of = factor_of * jnp.repeat(draws, extent[dim] // blocks).reshape([-1 if axis == dim else 1 for axis in range(len(extent))])
    return factor_of


def scatter_about(stream_key, dims, width, most, shards=(), kind=jnp.bfloat16):
    level = block_scale(stream_key, dims, shards, -0.22, 0.18) if shards else 1.0
    values = jax.random.normal(stream_key, dims, jnp.float32) * width * level
    return jnp.minimum(jnp.maximum(values, -most), most).astype(kind)


def setup_inputs(seed: int = 0, part: int = 0) -> dict:
    splits = jax.random.split(jax.random.key(seed), 13)
    own_keys = jax.random.split(jax.random.fold_in(splits[12], part), 13)
    return {
        "latent": draw_latent(jax.random.fold_in(jax.random.fold_in(splits[12], part), 71), part),
        "context": scatter_about(own_keys[1], (CTX, D), 1.0, 6.0, ((0, 4),)),
        "conditioning": scatter_about(own_keys[2], (D,), 1.5, 6.0, ((0, 4),)),
        "norm_gain": jnp.clip(1.0 + 0.18 * jax.random.normal(splits[3], (D,), jnp.float32), 0.1, 1.9),
        "shift_weight": scatter_about(splits[4], (D, D), D ** -0.5, 0.09375, ((0, 4), (1, 4))),
        "scale_weight": scatter_about(splits[5], (D, D), D ** -0.5, 0.09375, ((0, 4), (1, 4))),
        "gate_weight": scatter_about(splits[6], (D, D), D ** -0.5, 0.09375, ((0, 4), (1, 4))),
        "query_weight": draw_query_weight(jax.random.fold_in(splits[12], 71), part),
        "key_weight": draw_key_weight(jax.random.fold_in(splits[12], 71), part),
        "value_weight": scatter_about(splits[9], (D, KV_HEADS * HD), D ** -0.5, 0.09375, ((1, 4),)),
        "out_weight": scatter_about(splits[10], (HEADS * HD, D), (HD // 4) ** -0.5, 1.5, ((1, 4),)),
        "sink_logit": jnp.clip(3.0 + 4.0 * jax.random.uniform(splits[11], (HEADS,), jnp.float32) ** block_scale(splits[11], (HEADS,), ((0, 4),), -0.2, 0.2), 3.0, 7.0),
    }


epsilon = 1e-06
rope_base = 10000.0
neg_large = -1e+30

def row_norm(matrix, norm_gain):
    values = matrix.astype(jnp.float32)
    return values * lax.rsqrt(lax.optimization_barrier(jnp.mean(values * values, axis=-1, keepdims=True)) + epsilon) * norm_gain

def axial_turn(values, position):
    half_dim = values.shape[-1] // 2
    quarter = half_dim // 2
    inverse = rope_base ** (-jnp.arange(quarter, dtype=jnp.float32) / quarter)

    def turn(section, coordinate):
        angles = coordinate.astype(jnp.float32)[:, None] * inverse[None, :]
        cosine = jnp.cos(angles)[:, None, :]
        sine_part = jnp.sin(angles)[:, None, :]
        leading = section[..., :quarter]
        trailing = section[..., quarter:]
        return jnp.concatenate([leading * cosine - trailing * sine_part, leading * sine_part + trailing * cosine], axis=-1)
    return jnp.concatenate([turn(values[..., :half_dim], position // GRID_W), turn(values[..., half_dim:], position % GRID_W)], axis=-1)

def reference(latent, context, conditioning, norm_gain, shift_weight, scale_weight, gate_weight, query_weight, key_weight, value_weight, out_weight, sink_logit):
    lifted = jax.nn.silu(conditioning.astype(jnp.float32)).astype(jnp.bfloat16)[None, :]
    shift_vec = jnp.dot(lifted, shift_weight, preferred_element_type=jnp.float32)[0]
    scale_vec = jnp.dot(lifted, scale_weight, preferred_element_type=jnp.float32)[0]
    gate_vec = jnp.dot(lifted, gate_weight, preferred_element_type=jnp.float32)[0]
    normed = (row_norm(latent, norm_gain) * (1.0 + scale_vec) + shift_vec).astype(jnp.bfloat16)
    position = jnp.arange(SEQ, dtype=jnp.int32)
    queries = axial_turn(jnp.dot(normed, query_weight, preferred_element_type=jnp.float32).reshape(SEQ, HEADS, HD), position).astype(jnp.bfloat16)
    latent_keys = axial_turn(jnp.dot(normed, key_weight, preferred_element_type=jnp.float32).reshape(SEQ, KV_HEADS, HD), position).astype(jnp.bfloat16)
    latent_values = jnp.dot(normed, value_weight, preferred_element_type=jnp.float32).astype(jnp.bfloat16).reshape(SEQ, KV_HEADS, HD)
    prepared = row_norm(context, norm_gain).astype(jnp.bfloat16)
    context_keys = jnp.dot(prepared, key_weight, preferred_element_type=jnp.float32).astype(jnp.bfloat16).reshape(CTX, KV_HEADS, HD).astype(jnp.float32)
    context_values = jnp.dot(prepared, value_weight, preferred_element_type=jnp.float32).astype(jnp.bfloat16).reshape(CTX, KV_HEADS, HD).astype(jnp.float32)
    group_size = HEADS // KV_HEADS
    factor = HD ** (-0.5)
    padded_keys = jnp.pad(latent_keys, ((WIN, WIN), (0, 0), (0, 0)))
    padded_values = jnp.pad(latent_values, ((WIN, WIN), (0, 0), (0, 0)))
    sink_values = sink_logit.astype(jnp.float32).reshape(KV_HEADS, group_size)[:, :, None, None]

    def one_block(block_index):
        first_row = block_index * WIN
        block_queries = lax.dynamic_slice_in_dim(queries, first_row, WIN, 0).reshape(WIN, KV_HEADS, group_size, HD).astype(jnp.float32)
        block_keys = lax.dynamic_slice_in_dim(padded_keys, first_row, 3 * WIN, 0).astype(jnp.float32)
        block_values = lax.dynamic_slice_in_dim(padded_values, first_row, 3 * WIN, 0).astype(jnp.float32)
        local_scores = jnp.einsum('qhgd,khd->hgqk', block_queries, block_keys) * factor
        query_pos = first_row + jnp.arange(WIN, dtype=jnp.int32)
        key_pos = first_row - WIN + jnp.arange(3 * WIN, dtype=jnp.int32)
        allowed = (jnp.abs(key_pos[None, :] - query_pos[:, None]) <= WIN) & (key_pos[None, :] >= 0) & (key_pos[None, :] < SEQ)
        local_scores = jnp.where(allowed, local_scores, neg_large)
        context_scores = jnp.einsum('qhgd,thd->hgqt', block_queries, context_keys) * factor
        joined = jnp.concatenate([local_scores, context_scores, jnp.broadcast_to(sink_values, local_scores.shape[:-1] + (1,))], axis=-1)
        highest = lax.optimization_barrier(jnp.max(joined, axis=-1, keepdims=True))
        exponent = jnp.exp(joined - highest)
        weights = (exponent / lax.optimization_barrier(jnp.sum(exponent, axis=-1, keepdims=True))).astype(jnp.bfloat16)
        weights = lax.optimization_barrier(weights).astype(jnp.float32)
        out_block = jnp.einsum('hgqk,khd->qhgd', weights[..., :3 * WIN], block_values) + jnp.einsum('hgqt,thd->qhgd', weights[..., 3 * WIN:3 * WIN + CTX], context_values)
        return out_block.reshape(WIN, HEADS * HD).astype(jnp.bfloat16)
    attended = lax.map(one_block, jnp.arange(SEQ // WIN, dtype=jnp.int32)).reshape(SEQ, HEADS * HD)
    blended = jnp.dot(attended, out_weight, preferred_element_type=jnp.float32).astype(jnp.bfloat16)
    blended = lax.optimization_barrier(blended).astype(jnp.float32)
    return (latent.astype(jnp.float32) + gate_vec * blended).astype(jnp.bfloat16)
```

```python
import functools

import jax
import jax.numpy as jnp
from jax import lax
from jax.experimental import pallas as pl
from jax.experimental.pallas import tpu as pltpu
from jax.sharding import PartitionSpec as P

HEADS = 16
KV_HEADS = 8
HD = 64
GRID_W = 64
WIN = 128


epsilon = 1e-06
rope_base = 10000.0
neg_large = -1e30


def with_halo(cells, sides, width):
    for axis, dim in sides:
        count = lax.axis_size(axis)
        ends = count - 1
        head = lax.slice_in_dim(cells, 0, width, axis=dim)
        tail = lax.slice_in_dim(cells, cells.shape[dim] - width, cells.shape[dim], axis=dim)
        cells = jnp.concatenate(
            [
                lax.ppermute(tail, axis, [(i, (i + 1) % count) for i in range(ends)]),
                cells,
                lax.ppermute(head, axis, [((i + 1) % count, i) for i in range(ends)]),
            ],
            axis=dim,
        )
    return cells


def row_norm(matrix, norm_gain):
    values = matrix.astype(jnp.float32)
    return (
        values * lax.rsqrt(jnp.mean(values * values, axis=-1, keepdims=True) + epsilon) * norm_gain
    )


def axial_turn(values, position):
    half_dim = values.shape[-1] // 2
    quarter = half_dim // 2
    inverse = rope_base ** (-jnp.arange(quarter, dtype=jnp.float32) / quarter)

    def turn(section, coordinate):
        angles = coordinate.astype(jnp.float32)[:, None] * inverse[None, :]
        cosine = jnp.cos(angles)[:, None, :]
        sine_part = jnp.sin(angles)[:, None, :]
        leading = section[..., :quarter]
        trailing = section[..., quarter:]
        return jnp.concatenate(
            [leading * cosine - trailing * sine_part, leading * sine_part + trailing * cosine],
            axis=-1,
        )

    return jnp.concatenate(
        [
            turn(values[..., :half_dim], position // GRID_W),
            turn(values[..., half_dim:], position % GRID_W),
        ],
        axis=-1,
    )


def context_pairs(context_rows, norm_gain, key_weight, value_weight):
    prepared = row_norm(context_rows, norm_gain).astype(jnp.bfloat16)
    return jnp.concatenate(
        [
            jnp.dot(prepared, key_weight, preferred_element_type=jnp.float32),
            jnp.dot(prepared, value_weight, preferred_element_type=jnp.float32),
        ],
        axis=1,
    ).astype(jnp.bfloat16)


def local_plain(
    latent,
    context,
    conditioning,
    norm_gain,
    shift_weight,
    scale_weight,
    gate_weight,
    query_weight,
    key_weight,
    value_weight,
    out_weight,
    sink_logit,
):
    lifted = jax.nn.silu(conditioning.astype(jnp.float32)).astype(jnp.bfloat16)[None, :]
    shift_part = jnp.dot(lifted, shift_weight, preferred_element_type=jnp.float32)[0]
    scale_part = jnp.dot(lifted, scale_weight, preferred_element_type=jnp.float32)[0]
    gate_part = jnp.dot(lifted, gate_weight, preferred_element_type=jnp.float32)[0]
    summed = lax.psum((shift_part, scale_part, gate_part), "sp")
    shift_vec, scale_vec, gate_vec = (
        lax.all_gather(summed[0], "tp", axis=0, tiled=True),
        lax.all_gather(summed[1], "tp", axis=0, tiled=True),
        lax.all_gather(summed[2], "tp", axis=0, tiled=True),
    )
    normed = (row_norm(latent, norm_gain) * (1.0 + scale_vec) + shift_vec).astype(jnp.bfloat16)
    segment = lax.all_gather(normed, "tp", axis=0, tiled=True)
    projected = jnp.concatenate(
        [
            jnp.dot(segment, query_weight, preferred_element_type=jnp.float32),
            jnp.dot(segment, key_weight, preferred_element_type=jnp.float32),
            jnp.dot(segment, value_weight, preferred_element_type=jnp.float32),
        ],
        axis=1,
    )
    row_count = projected.shape[0]
    query_width = query_weight.shape[1]
    key_width = key_weight.shape[1]
    query_heads = query_width // HD
    pair_heads = key_width // HD
    group_size = HEADS // KV_HEADS
    row_offset = lax.axis_index("sp") * row_count
    position = row_offset + jnp.arange(row_count, dtype=jnp.int32)
    queries = axial_turn(
        projected[:, :query_width].reshape(row_count, query_heads, HD), position
    ).astype(jnp.bfloat16)
    latent_keys = axial_turn(
        projected[:, query_width : query_width + key_width].reshape(row_count, pair_heads, HD),
        position,
    ).astype(jnp.bfloat16)
    latent_values = projected[:, query_width + key_width :].astype(jnp.bfloat16)
    key_value = jnp.concatenate([latent_keys.reshape(row_count, key_width), latent_values], axis=1)
    widened = with_halo(key_value, (("sp", 0),), WIN)
    context_all = lax.all_gather(
        context_pairs(context, norm_gain, key_weight, value_weight), "sp", axis=0, tiled=True
    )
    block_count = row_count // WIN
    context_count = context_all.shape[0]
    query_blocks = queries.reshape(block_count, WIN, pair_heads, group_size, HD)
    band_blocks = widened.reshape(block_count + 2, WIN, 2 * key_width)
    band_rows = jnp.concatenate(
        [band_blocks[:block_count], band_blocks[1 : block_count + 1], band_blocks[2:]], axis=1
    )
    band_keys = band_rows[..., :key_width].reshape(block_count, 3 * WIN, pair_heads, HD)
    band_values = band_rows[..., key_width:].reshape(block_count, 3 * WIN, pair_heads, HD)
    context_keys = context_all[:, :key_width].reshape(context_count, pair_heads, HD)
    context_values = context_all[:, key_width:].reshape(context_count, pair_heads, HD)
    factor = HD ** (-0.5)
    local_scores = (
        jnp.einsum("nqhgd,nkhd->nhgqk", query_blocks, band_keys, preferred_element_type=jnp.float32)
        * factor
    )
    query_pos = position.reshape(block_count, WIN)
    key_pos = (
        row_offset
        - WIN
        + jnp.arange(block_count, dtype=jnp.int32)[:, None] * WIN
        + jnp.arange(3 * WIN, dtype=jnp.int32)[None, :]
    )
    seq_total = row_count * lax.axis_size("sp")
    allowed = (
        (jnp.abs(key_pos[:, None, :] - query_pos[:, :, None]) <= WIN)
        & (key_pos[:, None, :] >= 0)
        & (key_pos[:, None, :] < seq_total)
    )
    local_scores = jnp.where(allowed[:, None, None], local_scores, neg_large)
    context_scores = (
        jnp.einsum(
            "nqhgd,thd->nhgqt", query_blocks, context_keys, preferred_element_type=jnp.float32
        )
        * factor
    )
    sink_values = sink_logit.reshape(pair_heads, group_size)[None, :, :, None, None]
    highest = jnp.maximum(
        jnp.maximum(
            jnp.max(local_scores, axis=-1, keepdims=True),
            jnp.max(context_scores, axis=-1, keepdims=True),
        ),
        sink_values,
    )
    local_exp = jnp.exp(local_scores - highest)
    context_exp = jnp.exp(context_scores - highest)
    denominator = (
        jnp.sum(local_exp, axis=-1, keepdims=True)
        + jnp.sum(context_exp, axis=-1, keepdims=True)
        + jnp.exp(sink_values - highest)
    )
    local_weights = (local_exp / denominator).astype(jnp.bfloat16)
    context_weights = (context_exp / denominator).astype(jnp.bfloat16)
    attended = jnp.einsum(
        "nhgqk,nkhd->nqhgd", local_weights, band_values, preferred_element_type=jnp.float32
    ) + jnp.einsum(
        "nhgqt,thd->nqhgd", context_weights, context_values, preferred_element_type=jnp.float32
    )
    attended = attended.reshape(row_count, query_width).astype(jnp.bfloat16)
    columns_part = jnp.dot(
        lax.all_gather(attended, "tp", axis=1, tiled=True),
        out_weight,
        preferred_element_type=jnp.float32,
    ).astype(jnp.bfloat16)
    blended = lax.all_to_all(columns_part, "tp", split_axis=0, concat_axis=1, tiled=True)
    return (latent.astype(jnp.float32) + gate_vec * blended.astype(jnp.float32)).astype(
        jnp.bfloat16
    )


PIECES = 4
NORM_ROWS = 16


def remote(src, dst, send, recv, axis, peer):
    return pltpu.make_async_remote_copy(
        src_ref=src,
        dst_ref=dst,
        send_sem=send,
        recv_sem=recv,
        device_id={axis: peer},
        device_id_type=pl.DeviceIdType.MESH,
    )


def fused_kernel(
    tp,
    sp,
    latent,
    context,
    conditioning,
    norm_gain,
    shift_weight,
    scale_weight,
    gate_weight,
    query_weight,
    key_weight,
    value_weight,
    out_weight,
    sink,
    blended,
    gate_out,
    cond_v,
    gain_v,
    mod_w,
    wq,
    wk,
    wv,
    wo,
    ctx_v,
    rows_all,
    normed,
    mod_part,
    mod_all,
    factor_v,
    shift_v,
    gate_v,
    turn_cos,
    turn_sin,
    queries,
    key_value,
    ctx_kv,
    att_all,
    out_cols,
    load_sem,
    pair_send,
    pair_recv,
    far_send,
    far_recv,
    fwd_send,
    fwd_recv,
    modsp_send,
    modsp_recv,
    modtp_send,
    modtp_recv,
    ctx_send,
    ctx_recv,
    halo_send,
    halo_recv,
    apair_send,
    apair_recv,
    afar_send,
    afar_recv,
    afwd_send,
    afwd_recv,
    out_send,
    out_recv,
):
    t = lax.axis_index("tp")
    s = lax.axis_index("sp")
    chips = tp // 2
    core = lax.rem(t, 2)
    chip = t // 2
    pair = chip * 2 + (1 - core)
    rows, width = latent.shape
    ctx_rows = context.shape[0]
    mod_cols = shift_weight.shape[1]
    query_width = query_weight.shape[1]
    key_width = key_weight.shape[1]
    heads = query_width // HD
    group = heads // (key_width // HD)
    total = tp * rows
    out_width = out_weight.shape[1]
    piece = rows // PIECES
    f32, bf16 = jnp.float32, jnp.bfloat16

    def chip_at(j):
        return lax.rem(chip + j, chips)

    def chip_from(j):
        return lax.rem(chip + chips - j, chips)

    loads = [
        (conditioning, cond_v),
        (shift_weight, mod_w.at[0]),
        (scale_weight, mod_w.at[1]),
        (gate_weight, mod_w.at[2]),
        (norm_gain, gain_v),
        (context, ctx_v),
        (key_weight, wk),
        (value_weight, wv),
        (latent, rows_all.at[t]),
        (query_weight, wq),
        (out_weight, wo),
    ]
    loads = [pltpu.make_async_copy(a, b, load_sem.at[i]) for i, (a, b) in enumerate(loads)]
    for load in loads:
        load.start()

    barrier = pltpu.get_barrier_semaphore()
    for k in range(1, tp):
        pl.semaphore_signal(
            barrier, inc=1, device_id={"tp": lax.rem(t + k, tp)}, device_id_type=pl.DeviceIdType.MESH
        )
    for k in range(1, sp):
        pl.semaphore_signal(
            barrier, inc=1, device_id={"sp": lax.rem(s + k, sp)}, device_id_type=pl.DeviceIdType.MESH
        )
    pl.semaphore_wait(barrier, tp - 1 + sp - 1)

    far = {}
    for c in range(PIECES):
        part = pl.ds(c * piece, piece)
        for j in range(1, chips):
            i = (j - 1) * PIECES + c
            far[j, c] = remote(
                latent.at[part],
                rows_all.at[t, part],
                far_send.at[i],
                far_recv.at[i],
                "tp",
                chip_at(j) * 2 + core,
            )
            far[j, c].start()
    near = remote(latent, rows_all.at[t], pair_send.at[0], pair_recv.at[0], "tp", pair)
    near.start()

    for i in range(4):
        loads[i].wait()
    cond = cond_v[...].astype(f32)
    lifted = jnp.broadcast_to(cond / (1.0 + jnp.exp(-cond)), (16, cond.shape[1])).astype(bf16)
    for i in range(3):
        mod_part[s, :, i * mod_cols : (i + 1) * mod_cols] = jnp.dot(
            lifted, mod_w[i], preferred_element_type=f32
        )[0:1]
    mods = []
    for k in range(1, sp):
        copy = remote(
            mod_part.at[s],
            mod_part.at[s],
            modsp_send.at[k - 1],
            modsp_recv.at[k - 1],
            "sp",
            lax.rem(s + k, sp),
        )
        copy.start()
        mods.append(copy)

    for i in range(4, 8):
        loads[i].wait()

    def norm_context(g, carry):
        part = pl.ds(pl.multiple_of(g * NORM_ROWS, NORM_ROWS), NORM_ROWS)
        values = ctx_v[part].astype(f32)
        scale = lax.rsqrt(jnp.mean(values * values, axis=-1, keepdims=True) + epsilon)
        ctx_v[part] = (values * scale * gain_v[...]).astype(bf16)
        return carry

    lax.fori_loop(0, ctx_rows // NORM_ROWS, norm_context, 0)
    ctx_kv[s, :, :key_width] = jnp.dot(ctx_v[...], wk[...], preferred_element_type=f32).astype(bf16)
    ctx_kv[s, :, key_width:] = jnp.dot(ctx_v[...], wv[...], preferred_element_type=f32).astype(bf16)
    ctxs = []
    for k in range(1, sp):
        copy = remote(
            ctx_kv.at[s],
            ctx_kv.at[s],
            ctx_send.at[k - 1],
            ctx_recv.at[k - 1],
            "sp",
            lax.rem(s + k, sp),
        )
        copy.start()
        ctxs.append(copy)

    for copy in mods:
        copy.wait()
    summed = mod_part[0]
    for k in range(1, sp):
        summed = summed + mod_part[k]
    mod_all[t] = summed
    mods = []
    for k in range(1, tp):
        copy = remote(
            mod_all.at[t],
            mod_all.at[t],
            modtp_send.at[k - 1],
            modtp_recv.at[k - 1],
            "tp",
            lax.rem(t + k, tp),
        )
        copy.start()
        mods.append(copy)

    lane = lax.broadcasted_iota(jnp.int32, (WIN, 128), 1)
    row = lax.broadcasted_iota(jnp.int32, (WIN, 128), 0)
    quarter = HD // 4
    inverse = jnp.exp(
        lax.rem(lane, quarter).astype(f32) * (-jnp.log(jnp.float32(rope_base)) / quarter)
    )
    first = lax.rem(lane, 2 * quarter) < quarter

    def tables(b, carry):
        place = s * total + b * WIN + row
        by_row = lax.rem(lane, HD) < HD // 2
        coordinate = jnp.where(by_row, place // GRID_W, lax.rem(place, GRID_W))
        angles = coordinate.astype(f32) * inverse
        turn_cos[b] = jnp.cos(angles)
        sines = jnp.sin(angles)
        turn_sin[b] = jnp.where(first, -sines, sines)
        return carry

    lax.fori_loop(0, tp, tables, 0)

    for copy in mods:
        copy.wait()
    for i in range(tp):
        cols = slice(i * mod_cols, (i + 1) * mod_cols)
        shift_v[:, cols] = mod_all[i, :, 0:mod_cols]
        factor_v[:, cols] = gain_v[:, cols] * (1.0 + mod_all[i, :, mod_cols : 2 * mod_cols])
        gate_v[:, cols] = mod_all[i, :, 2 * mod_cols : 3 * mod_cols]
    gate_store = pltpu.make_async_copy(gate_v, gate_out, load_sem.at[len(loads)])
    gate_store.start()

    low = lane < HD

    def turned(values, slot):
        swapped = jnp.where(
            first, pltpu.roll(values, 128 - quarter, 1), pltpu.roll(values, quarter, 1)
        )
        return values * turn_cos[slot] + swapped * turn_sin[slot]

    def project(slot):
        def norm_rows(g, carry):
            part = pl.ds(pl.multiple_of(g * NORM_ROWS, NORM_ROWS), NORM_ROWS)
            values = rows_all[slot, part].astype(f32)
            scale = lax.rsqrt(jnp.mean(values * values, axis=-1, keepdims=True) + epsilon)
            normed[part] = (values * scale * factor_v[...] + shift_v[...]).astype(bf16)
            return carry

        lax.fori_loop(0, rows // NORM_ROWS, norm_rows, 0)
        base = pl.multiple_of(WIN + slot * rows, WIN)
        prepared = normed[...]
        q = jnp.dot(prepared, wq[...], preferred_element_type=f32)
        k = jnp.dot(prepared, wk[...], preferred_element_type=f32)
        v = jnp.dot(prepared, wv[...], preferred_element_type=f32)
        key_value[pl.ds(base, rows), :key_width] = turned(k, slot).astype(bf16)
        key_value[pl.ds(base, rows), key_width:] = v.astype(bf16)
        factor = HD ** (-0.5)
        for h in range(heads):
            lanes = q[:, (h // 2) * 128 : (h // 2 + 1) * 128]
            lanes = (turned(lanes, slot).astype(bf16).astype(f32)) * factor
            at, want = h % 2, h // group
            if at != want:
                lanes = pltpu.roll(lanes, HD, 1)
            keep = low if want == 0 else jnp.logical_not(low)
            queries[slot, h * rows : (h + 1) * rows] = jnp.where(keep, lanes, 0.0).astype(bf16)

    loads[8].wait()
    loads[9].wait()

    def fwd(j, c):
        slot = chip_from(j) * 2 + core
        part = pl.ds(c * piece, piece)
        i = (j - 1) * PIECES + c
        return remote(
            rows_all.at[slot, part],
            rows_all.at[slot, part],
            fwd_send.at[i],
            fwd_recv.at[i],
            "tp",
            pair,
        )

    def project_step(k, carry):
        @pl.when(k == 1)
        def _():
            near.wait_recv()

        for j in range(1, chips):

            @pl.when(k == 2 * j)
            def _():
                for c in range(PIECES):
                    far[j, c].wait_recv()
                    fwd(j, c).start()

            @pl.when(k == 2 * j + 1)
            def _():
                for c in range(PIECES):
                    fwd(j, c).wait_recv()

        source = lax.rem(chip + chips - k // 2, chips)
        flip = lax.rem(k, 2)
        project(source * 2 + core + flip - 2 * core * flip)
        return carry

    lax.fori_loop(0, tp, project_step, 0)

    halo_right = remote(
        key_value.at[pl.ds(total, WIN)],
        key_value.at[pl.ds(0, WIN)],
        halo_send.at[0],
        halo_recv.at[0],
        "sp",
        lax.rem(s + 1, sp),
    )
    halo_left = remote(
        key_value.at[pl.ds(WIN, WIN)],
        key_value.at[pl.ds(total + WIN, WIN)],
        halo_send.at[1],
        halo_recv.at[1],
        "sp",
        lax.rem(s + sp - 1, sp),
    )
    halo_right.start()
    halo_left.start()
    for copy in ctxs:
        copy.wait()
    loads[10].wait()

    def block_at(step):
        return jnp.where(step < tp - 1, lax.rem(step + 1, tp - 1), tp - 1)

    def att_pair(b):
        return remote(
            att_all.at[b, t], att_all.at[b, t], apair_send.at[b], apair_recv.at[b], "tp", pair
        )

    def att_far(b, j):
        i = b * (chips - 1) + j - 1
        return remote(
            att_all.at[b, t],
            att_all.at[b, t],
            afar_send.at[i],
            afar_recv.at[i],
            "tp",
            chip_at(j) * 2 + core,
        )

    def att_fwd(b, j):
        slot = chip_from(j) * 2 + core
        i = b * (chips - 1) + j - 1
        return remote(
            att_all.at[b, slot],
            att_all.at[b, slot],
            afwd_send.at[i],
            afwd_recv.at[i],
            "tp",
            pair,
        )

    contract = (((1,), (1,)), ((), ()))
    band = 3 * WIN
    q_pos = lax.broadcasted_iota(jnp.int32, (WIN, band), 0)
    k_pos = lax.broadcasted_iota(jnp.int32, (WIN, band), 1)
    in_window = jnp.logical_and(k_pos >= q_pos, k_pos <= q_pos + 2 * WIN)

    def attend(b):
        start = pl.multiple_of(b * WIN, WIN)
        band_k = key_value[pl.ds(start, band), :key_width]
        band_v = key_value[pl.ds(start, band), key_width:]
        ctx_k = ctx_kv[:, :, :key_width].reshape(sp * ctx_rows, key_width)
        ctx_v_ = ctx_kv[:, :, key_width:].reshape(sp * ctx_rows, key_width)
        place = s * total + b * WIN - WIN + k_pos
        allowed = jnp.logical_and(
            in_window, jnp.logical_and(place >= 0, place < sp * total)
        )
        results = []
        for h in range(heads):
            q = queries[b, h * rows : (h + 1) * rows]
            near_s = lax.dot_general(q, band_k, contract, preferred_element_type=f32)
            near_s = jnp.where(allowed, near_s, neg_large)
            ctx_s = lax.dot_general(q, ctx_k, contract, preferred_element_type=f32)
            top = jnp.maximum(
                jnp.max(near_s, axis=-1, keepdims=True), jnp.max(ctx_s, axis=-1, keepdims=True)
            )
            top = jnp.maximum(top, sink[h])
            near_e = jnp.exp(near_s - top)
            ctx_e = jnp.exp(ctx_s - top)
            bottom = (
                jnp.sum(near_e, axis=-1, keepdims=True)
                + jnp.sum(ctx_e, axis=-1, keepdims=True)
                + jnp.exp(sink[h] - top)
            )
            share = 1.0 / bottom
            results.append(
                jnp.dot((near_e * share).astype(bf16), band_v, preferred_element_type=f32)
                + jnp.dot((ctx_e * share).astype(bf16), ctx_v_, preferred_element_type=f32)
            )
        for v in range(query_width // 128):
            sides = []
            for at in range(2):
                h = 2 * v + at
                lanes = results[h]
                if h // group != at:
                    lanes = pltpu.roll(lanes, HD, 1)
                sides.append(lanes)
            att_all[b, t, :, v * 128 : (v + 1) * 128] = jnp.where(low, sides[0], sides[1]).astype(
                bf16
            )

    def hand_on(b):
        for j in range(1, chips):
            att_far(b, j).wait_recv()
            att_fwd(b, j).start()

    def out_copy(b):
        return remote(
            out_cols.at[b],
            blended.at[:, pl.ds(pl.multiple_of(t * out_width, 128), out_width)],
            out_send.at[b],
            out_recv.at[t],
            "tp",
            b,
        )

    own_copy = pltpu.make_async_copy(
        out_cols.at[t],
        blended.at[:, pl.ds(pl.multiple_of(t * out_width, 128), out_width)],
        load_sem.at[len(loads) + 1],
    )

    def finish(b):
        att_pair(b).wait_recv()
        for j in range(1, chips):
            att_fwd(b, j).wait_recv()
        sums = jnp.dot(att_all[b, 0], wo[0:query_width], preferred_element_type=f32)
        for i in range(1, tp):
            sums = sums + jnp.dot(
                att_all[b, i],
                wo[i * query_width : (i + 1) * query_width],
                preferred_element_type=f32,
            )
        out_cols[b] = sums.astype(bf16)

        @pl.when(b == t)
        def _():
            own_copy.start()

        @pl.when(b != t)
        def _():
            out_copy(b).start()

    def attend_step(step, carry):
        @pl.when(step < tp)
        def _():
            b = block_at(step)

            @pl.when(step == tp - 2)
            def _():
                halo_right.wait_recv()

            @pl.when(step == tp - 1)
            def _():
                halo_left.wait_recv()

            attend(b)
            att_pair(b).start()
            for j in range(1, chips):
                att_far(b, j).start()

        @pl.when(jnp.logical_and(step >= 1, step < tp + 1))
        def _():
            hand_on(block_at(step - 1))

        @pl.when(step >= 2)
        def _():
            finish(block_at(step - 2))

        return carry

    lax.fori_loop(0, tp + 2, attend_step, 0)

    near.wait_send()
    for copy in far.values():
        copy.wait_send()
    for j in range(1, chips):
        for c in range(PIECES):
            fwd(j, c).wait_send()
    gate_store.wait()
    halo_right.wait_send()
    halo_left.wait_send()
    for b in range(tp):
        att_pair(b).wait_send()
        for j in range(1, chips):
            att_far(b, j).wait_send()
            att_fwd(b, j).wait_send()
    own_copy.wait()
    for k in range(1, tp):
        other = lax.rem(t + k, tp)
        out_copy(other).wait_send()
        remote(
            out_cols.at[other],
            blended.at[:, pl.ds(pl.multiple_of(other * out_width, 128), out_width)],
            out_send.at[other],
            out_recv.at[other],
            "tp",
            other,
        ).wait_recv()


def local(
    latent,
    context,
    conditioning,
    norm_gain,
    shift_weight,
    scale_weight,
    gate_weight,
    query_weight,
    key_weight,
    value_weight,
    out_weight,
    sink_logit,
):
    tp, sp = lax.axis_size("tp"), lax.axis_size("sp")
    rows, width = latent.shape
    ctx_rows = context.shape[0]
    mod_rows, mod_cols = shift_weight.shape
    query_width, key_width = query_weight.shape[1], key_weight.shape[1]
    out_width = out_weight.shape[1]
    fits = (
        rows == WIN
        and key_width == 2 * HD
        and tp % 2 == 0
        and tp >= 4
        and sp >= 2
        and ctx_rows % NORM_ROWS == 0
        and mod_cols % 128 == 0
    )
    if not fits:
        return local_plain(
            latent,
            context,
            conditioning,
            norm_gain,
            shift_weight,
            scale_weight,
            gate_weight,
            query_weight,
            key_weight,
            value_weight,
            out_weight,
            sink_logit,
        )
    f32, bf16 = jnp.float32, jnp.bfloat16
    chips = tp // 2
    far = (chips - 1) * PIECES
    dma = pltpu.SemaphoreType.DMA
    anywhere = pl.BlockSpec(memory_space=pl.ANY)
    blended, gate = pl.pallas_call(
        functools.partial(fused_kernel, tp, sp),
        out_shape=(
            jax.ShapeDtypeStruct((rows, width), bf16),
            jax.ShapeDtypeStruct((1, width), f32),
        ),
        in_specs=[anywhere] * 11 + [pl.BlockSpec(memory_space=pltpu.SMEM)],
        out_specs=(anywhere, anywhere),
        scratch_shapes=[
            pltpu.VMEM((1, mod_rows), bf16),
            pltpu.VMEM((1, width), f32),
            pltpu.VMEM((3, mod_rows, mod_cols), bf16),
            pltpu.VMEM(query_weight.shape, bf16),
            pltpu.VMEM(key_weight.shape, bf16),
            pltpu.VMEM(value_weight.shape, bf16),
            pltpu.VMEM(out_weight.shape, bf16),
            pltpu.VMEM(context.shape, bf16),
            pltpu.VMEM((tp, rows, width), bf16),
            pltpu.VMEM((rows, width), bf16),
            pltpu.VMEM((sp, 1, 3 * mod_cols), f32),
            pltpu.VMEM((tp, 1, 3 * mod_cols), f32),
            pltpu.VMEM((1, width), f32),
            pltpu.VMEM((1, width), f32),
            pltpu.VMEM((1, width), f32),
            pltpu.VMEM((tp, rows, 128), f32),
            pltpu.VMEM((tp, rows, 128), f32),
            pltpu.VMEM((tp, query_width // HD * rows, key_width), bf16),
            pltpu.VMEM(((tp + 2) * rows, 2 * key_width), bf16),
            pltpu.VMEM((sp, ctx_rows, 2 * key_width), bf16),
            pltpu.VMEM((tp, tp, rows, query_width), bf16),
            pltpu.VMEM((tp, rows, out_width), bf16),
            dma((13,)),
            dma((1,)),
            dma((1,)),
            dma((far,)),
            dma((far,)),
            dma((far,)),
            dma((far,)),
            dma((sp - 1,)),
            dma((sp - 1,)),
            dma((tp - 1,)),
            dma((tp - 1,)),
            dma((sp - 1,)),
            dma((sp - 1,)),
            dma((2,)),
            dma((2,)),
            dma((tp,)),
            dma((tp,)),
            dma((tp * (chips - 1),)),
            dma((tp * (chips - 1),)),
            dma((tp * (chips - 1),)),
            dma((tp * (chips - 1),)),
            dma((tp,)),
            dma((tp,)),
        ],
        compiler_params=pltpu.CompilerParams(
            collective_id=0, has_side_effects=True, vmem_limit_bytes=60 * 1024 * 1024
        ),
        name="fused",
    )(
        latent,
        context,
        conditioning.reshape(1, mod_rows),
        norm_gain.reshape(1, width),
        shift_weight,
        scale_weight,
        gate_weight,
        query_weight,
        key_weight,
        value_weight,
        out_weight,
        sink_logit,
    )
    return (latent.astype(f32) + gate * blended.astype(f32)).astype(bf16)


def solution(mesh):
    in_specs = (
        P(("grp", "sp", "tp"), None),
        P(("grp", "sp"), None),
        P(("grp", "sp")),
        P(),
        P("sp", "tp"),
        P("sp", "tp"),
        P("sp", "tp"),
        P(None, "tp"),
        P(None, "tp"),
        P(None, "tp"),
        P(None, "tp"),
        P("tp"),
    )
    out_specs = P(("grp", "sp", "tp"), None)
    return jax.shard_map(local, mesh=mesh, in_specs=in_specs, out_specs=out_specs, check_vma=False)
```

```python
import functools

import jax
import jax.numpy as jnp
from jax import lax
from jax.experimental import pallas as pl
from jax.experimental.pallas import tpu as pltpu
from jax.sharding import PartitionSpec as P

HEADS = 16
KV_HEADS = 8
HD = 64
GRID_W = 64
WIN = 128


epsilon = 1e-06
rope_base = 10000.0
neg_large = -1e30


def with_halo(cells, sides, width):
    for axis, dim in sides:
        count = lax.axis_size(axis)
        ends = count - 1
        head = lax.slice_in_dim(cells, 0, width, axis=dim)
        tail = lax.slice_in_dim(cells, cells.shape[dim] - width, cells.shape[dim], axis=dim)
        cells = jnp.concatenate(
            [
                lax.ppermute(tail, axis, [(i, (i + 1) % count) for i in range(ends)]),
                cells,
                lax.ppermute(head, axis, [((i + 1) % count, i) for i in range(ends)]),
            ],
            axis=dim,
        )
    return cells


def row_norm(matrix, norm_gain):
    values = matrix.astype(jnp.float32)
    return (
        values * lax.rsqrt(jnp.mean(values * values, axis=-1, keepdims=True) + epsilon) * norm_gain
    )


def axial_turn(values, position):
    half_dim = values.shape[-1] // 2
    quarter = half_dim // 2
    inverse = rope_base ** (-jnp.arange(quarter, dtype=jnp.float32) / quarter)

    def turn(section, coordinate):
        angles = coordinate.astype(jnp.float32)[:, None] * inverse[None, :]
        cosine = jnp.cos(angles)[:, None, :]
        sine_part = jnp.sin(angles)[:, None, :]
        leading = section[..., :quarter]
        trailing = section[..., quarter:]
        return jnp.concatenate(
            [leading * cosine - trailing * sine_part, leading * sine_part + trailing * cosine],
            axis=-1,
        )

    return jnp.concatenate(
        [
            turn(values[..., :half_dim], position // GRID_W),
            turn(values[..., half_dim:], position % GRID_W),
        ],
        axis=-1,
    )


def context_pairs(context_rows, norm_gain, key_weight, value_weight):
    prepared = row_norm(context_rows, norm_gain).astype(jnp.bfloat16)
    return jnp.concatenate(
        [
            jnp.dot(prepared, key_weight, preferred_element_type=jnp.float32),
            jnp.dot(prepared, value_weight, preferred_element_type=jnp.float32),
        ],
        axis=1,
    ).astype(jnp.bfloat16)


def local_plain(
    latent,
    context,
    conditioning,
    norm_gain,
    shift_weight,
    scale_weight,
    gate_weight,
    query_weight,
    key_weight,
    value_weight,
    out_weight,
    sink_logit,
):
    lifted = jax.nn.silu(conditioning.astype(jnp.float32)).astype(jnp.bfloat16)[None, :]
    shift_part = jnp.dot(lifted, shift_weight, preferred_element_type=jnp.float32)[0]
    scale_part = jnp.dot(lifted, scale_weight, preferred_element_type=jnp.float32)[0]
    gate_part = jnp.dot(lifted, gate_weight, preferred_element_type=jnp.float32)[0]
    summed = lax.psum((shift_part, scale_part, gate_part), "sp")
    shift_vec, scale_vec, gate_vec = (
        lax.all_gather(summed[0], "tp", axis=0, tiled=True),
        lax.all_gather(summed[1], "tp", axis=0, tiled=True),
        lax.all_gather(summed[2], "tp", axis=0, tiled=True),
    )
    normed = (row_norm(latent, norm_gain) * (1.0 + scale_vec) + shift_vec).astype(jnp.bfloat16)
    segment = lax.all_gather(normed, "tp", axis=0, tiled=True)
    projected = jnp.concatenate(
        [
            jnp.dot(segment, query_weight, preferred_element_type=jnp.float32),
            jnp.dot(segment, key_weight, preferred_element_type=jnp.float32),
            jnp.dot(segment, value_weight, preferred_element_type=jnp.float32),
        ],
        axis=1,
    )
    row_count = projected.shape[0]
    query_width = query_weight.shape[1]
    key_width = key_weight.shape[1]
    query_heads = query_width // HD
    pair_heads = key_width // HD
    group_size = HEADS // KV_HEADS
    row_offset = lax.axis_index("sp") * row_count
    position = row_offset + jnp.arange(row_count, dtype=jnp.int32)
    queries = axial_turn(
        projected[:, :query_width].reshape(row_count, query_heads, HD), position
    ).astype(jnp.bfloat16)
    latent_keys = axial_turn(
        projected[:, query_width : query_width + key_width].reshape(row_count, pair_heads, HD),
        position,
    ).astype(jnp.bfloat16)
    latent_values = projected[:, query_width + key_width :].astype(jnp.bfloat16)
    key_value = jnp.concatenate([latent_keys.reshape(row_count, key_width), latent_values], axis=1)
    widened = with_halo(key_value, (("sp", 0),), WIN)
    context_all = lax.all_gather(
        context_pairs(context, norm_gain, key_weight, value_weight), "sp", axis=0, tiled=True
    )
    block_count = row_count // WIN
    context_count = context_all.shape[0]
    query_blocks = queries.reshape(block_count, WIN, pair_heads, group_size, HD)
    band_blocks = widened.reshape(block_count + 2, WIN, 2 * key_width)
    band_rows = jnp.concatenate(
        [band_blocks[:block_count], band_blocks[1 : block_count + 1], band_blocks[2:]], axis=1
    )
    band_keys = band_rows[..., :key_width].reshape(block_count, 3 * WIN, pair_heads, HD)
    band_values = band_rows[..., key_width:].reshape(block_count, 3 * WIN, pair_heads, HD)
    context_keys = context_all[:, :key_width].reshape(context_count, pair_heads, HD)
    context_values = context_all[:, key_width:].reshape(context_count, pair_heads, HD)
    factor = HD ** (-0.5)
    local_scores = (
        jnp.einsum("nqhgd,nkhd->nhgqk", query_blocks, band_keys, preferred_element_type=jnp.float32)
        * factor
    )
    query_pos = position.reshape(block_count, WIN)
    key_pos = (
        row_offset
        - WIN
        + jnp.arange(block_count, dtype=jnp.int32)[:, None] * WIN
        + jnp.arange(3 * WIN, dtype=jnp.int32)[None, :]
    )
    seq_total = row_count * lax.axis_size("sp")
    allowed = (
        (jnp.abs(key_pos[:, None, :] - query_pos[:, :, None]) <= WIN)
        & (key_pos[:, None, :] >= 0)
        & (key_pos[:, None, :] < seq_total)
    )
    local_scores = jnp.where(allowed[:, None, None], local_scores, neg_large)
    context_scores = (
        jnp.einsum(
            "nqhgd,thd->nhgqt", query_blocks, context_keys, preferred_element_type=jnp.float32
        )
        * factor
    )
    sink_values = sink_logit.reshape(pair_heads, group_size)[None, :, :, None, None]
    highest = jnp.maximum(
        jnp.maximum(
            jnp.max(local_scores, axis=-1, keepdims=True),
            jnp.max(context_scores, axis=-1, keepdims=True),
        ),
        sink_values,
    )
    local_exp = jnp.exp(local_scores - highest)
    context_exp = jnp.exp(context_scores - highest)
    denominator = (
        jnp.sum(local_exp, axis=-1, keepdims=True)
        + jnp.sum(context_exp, axis=-1, keepdims=True)
        + jnp.exp(sink_values - highest)
    )
    local_weights = (local_exp / denominator).astype(jnp.bfloat16)
    context_weights = (context_exp / denominator).astype(jnp.bfloat16)
    attended = jnp.einsum(
        "nhgqk,nkhd->nqhgd", local_weights, band_values, preferred_element_type=jnp.float32
    ) + jnp.einsum(
        "nhgqt,thd->nqhgd", context_weights, context_values, preferred_element_type=jnp.float32
    )
    attended = attended.reshape(row_count, query_width).astype(jnp.bfloat16)
    columns_part = jnp.dot(
        lax.all_gather(attended, "tp", axis=1, tiled=True),
        out_weight,
        preferred_element_type=jnp.float32,
    ).astype(jnp.bfloat16)
    blended = lax.all_to_all(columns_part, "tp", split_axis=0, concat_axis=1, tiled=True)
    return (latent.astype(jnp.float32) + gate_vec * blended.astype(jnp.float32)).astype(
        jnp.bfloat16
    )


PIECES = 4
NORM_ROWS = 16


def remote(src, dst, send, recv, axis, peer):
    return pltpu.make_async_remote_copy(
        src_ref=src,
        dst_ref=dst,
        send_sem=send,
        recv_sem=recv,
        device_id={axis: peer},
        device_id_type=pl.DeviceIdType.MESH,
    )


def fused_kernel(
    tp,
    sp,
    latent,
    context,
    conditioning,
    norm_gain,
    shift_weight,
    scale_weight,
    gate_weight,
    query_weight,
    key_weight,
    value_weight,
    out_weight,
    sink,
    blended,
    gate_out,
    cond_v,
    gain_v,
    mod_w,
    wq,
    wk,
    wv,
    wo,
    ctx_v,
    rows_all,
    normed,
    mod_part,
    mod_all,
    factor_v,
    shift_v,
    gate_v,
    turn_cos,
    turn_sin,
    queries,
    key_value,
    ctx_kv,
    att_all,
    out_cols,
    load_sem,
    pair_send,
    pair_recv,
    far_send,
    far_recv,
    fwd_send,
    fwd_recv,
    modsp_send,
    modsp_recv,
    modtp_send,
    modtp_recv,
    ctx_send,
    ctx_recv,
    halo_send,
    halo_recv,
    apair_send,
    apair_recv,
    afar_send,
    afar_recv,
    afwd_send,
    afwd_recv,
    out_send,
    out_recv,
):
    t = lax.axis_index("tp")
    s = lax.axis_index("sp")
    chips = tp // 2
    core = lax.rem(t, 2)
    chip = t // 2
    pair = chip * 2 + (1 - core)
    rows, width = latent.shape
    ctx_rows = context.shape[0]
    mod_cols = shift_weight.shape[1]
    query_width = query_weight.shape[1]
    key_width = key_weight.shape[1]
    heads = query_width // HD
    group = heads // (key_width // HD)
    total = tp * rows
    out_width = out_weight.shape[1]
    piece = rows // PIECES
    f32, bf16 = jnp.float32, jnp.bfloat16

    def chip_at(j):
        return lax.rem(chip + j, chips)

    def chip_from(j):
        return lax.rem(chip + chips - j, chips)

    loads = [
        (conditioning, cond_v),
        (shift_weight, mod_w.at[0]),
        (scale_weight, mod_w.at[1]),
        (gate_weight, mod_w.at[2]),
        (norm_gain, gain_v),
        (context, ctx_v),
        (key_weight, wk),
        (value_weight, wv),
        (latent, rows_all.at[t]),
        (query_weight, wq),
        (out_weight, wo),
    ]
    loads = [pltpu.make_async_copy(a, b, load_sem.at[i]) for i, (a, b) in enumerate(loads)]
    for load in loads:
        load.start()

    barrier = pltpu.get_barrier_semaphore()
    for k in range(1, tp):
        pl.semaphore_signal(
            barrier, inc=1, device_id={"tp": lax.rem(t + k, tp)}, device_id_type=pl.DeviceIdType.MESH
        )
    for k in range(1, sp):
        pl.semaphore_signal(
            barrier, inc=1, device_id={"sp": lax.rem(s + k, sp)}, device_id_type=pl.DeviceIdType.MESH
        )
    pl.semaphore_wait(barrier, tp - 1 + sp - 1)

    far = {}
    for c in range(PIECES):
        part = pl.ds(c * piece, piece)
        for j in range(1, chips):
            i = (j - 1) * PIECES + c
            far[j, c] = remote(
                latent.at[part],
                rows_all.at[t, part],
                far_send.at[i],
                far_recv.at[i],
                "tp",
                chip_at(j) * 2 + core,
            )
            far[j, c].start()
    near = remote(latent, rows_all.at[t], pair_send.at[0], pair_recv.at[0], "tp", pair)
    near.start()

    for i in range(4):
        loads[i].wait()
    cond = cond_v[...].astype(f32).reshape(1, cond_v.shape[0])
    lifted = jnp.broadcast_to(cond / (1.0 + jnp.exp(-cond)), (16, cond.shape[1])).astype(bf16)
    for i in range(3):
        mod_part[s, :, i * mod_cols : (i + 1) * mod_cols] = jnp.dot(
            lifted, mod_w[i], preferred_element_type=f32
        )[0:1]
    mods = []
    for k in range(1, sp):
        copy = remote(
            mod_part.at[s],
            mod_part.at[s],
            modsp_send.at[k - 1],
            modsp_recv.at[k - 1],
            "sp",
            lax.rem(s + k, sp),
        )
        copy.start()
        mods.append(copy)

    for i in range(4, 8):
        loads[i].wait()

    def norm_context(g, carry):
        part = pl.ds(pl.multiple_of(g * NORM_ROWS, NORM_ROWS), NORM_ROWS)
        values = ctx_v[part].astype(f32)
        scale = lax.rsqrt(jnp.mean(values * values, axis=-1, keepdims=True) + epsilon)
        ctx_v[part] = (values * scale * gain_v[...]).astype(bf16)
        return carry

    lax.fori_loop(0, ctx_rows // NORM_ROWS, norm_context, 0)
    ctx_kv[s, :, :key_width] = jnp.dot(ctx_v[...], wk[...], preferred_element_type=f32).astype(bf16)
    ctx_kv[s, :, key_width:] = jnp.dot(ctx_v[...], wv[...], preferred_element_type=f32).astype(bf16)
    ctxs = []
    for k in range(1, sp):
        copy = remote(
            ctx_kv.at[s],
            ctx_kv.at[s],
            ctx_send.at[k - 1],
            ctx_recv.at[k - 1],
            "sp",
            lax.rem(s + k, sp),
        )
        copy.start()
        ctxs.append(copy)

    for copy in mods:
        copy.wait()
    summed = mod_part[0]
    for k in range(1, sp):
        summed = summed + mod_part[k]
    mod_all[t] = summed
    mods = []
    for k in range(1, tp):
        copy = remote(
            mod_all.at[t],
            mod_all.at[t],
            modtp_send.at[k - 1],
            modtp_recv.at[k - 1],
            "tp",
            lax.rem(t + k, tp),
        )
        copy.start()
        mods.append(copy)

    lane = lax.broadcasted_iota(jnp.int32, (WIN, 128), 1)
    row = lax.broadcasted_iota(jnp.int32, (WIN, 128), 0)
    quarter = HD // 4
    inverse = jnp.exp(
        lax.rem(lane, quarter).astype(f32) * (-jnp.log(jnp.float32(rope_base)) / quarter)
    )
    first = lax.rem(lane, 2 * quarter) < quarter

    def tables(b, carry):
        place = s * total + b * WIN + row
        by_row = lax.rem(lane, HD) < HD // 2
        coordinate = jnp.where(by_row, place // GRID_W, lax.rem(place, GRID_W))
        angles = coordinate.astype(f32) * inverse
        turn_cos[b] = jnp.cos(angles)
        sines = jnp.sin(angles)
        turn_sin[b] = jnp.where(first, -sines, sines)
        return carry

    lax.fori_loop(0, tp, tables, 0)

    for copy in mods:
        copy.wait()
    for i in range(tp):
        cols = slice(i * mod_cols, (i + 1) * mod_cols)
        shift_v[:, cols] = mod_all[i, :, 0:mod_cols]
        factor_v[:, cols] = gain_v[:, cols] * (1.0 + mod_all[i, :, mod_cols : 2 * mod_cols])
        gate_v[:, cols] = mod_all[i, :, 2 * mod_cols : 3 * mod_cols]
    gate_store = pltpu.make_async_copy(gate_v, gate_out, load_sem.at[len(loads)])
    gate_store.start()

    low = lane < HD

    def turned(values, slot):
        swapped = jnp.where(
            first, pltpu.roll(values, 128 - quarter, 1), pltpu.roll(values, quarter, 1)
        )
        return values * turn_cos[slot] + swapped * turn_sin[slot]

    half = rows // 2

    def norm_piece(slot, first_row, count, target):
        def norm_rows(g, carry):
            at = pl.multiple_of(first_row + g * NORM_ROWS, NORM_ROWS)
            values = rows_all[slot, pl.ds(at, NORM_ROWS)].astype(f32)
            scale = lax.rsqrt(jnp.mean(values * values, axis=-1, keepdims=True) + epsilon)
            normed[pl.ds(pl.multiple_of(target + at, NORM_ROWS), NORM_ROWS)] = (
                values * scale * factor_v[...] + shift_v[...]
            ).astype(bf16)
            return carry

        lax.fori_loop(0, count // NORM_ROWS, norm_rows, 0)

    def project(slots):
        prepared = normed[...]
        q_both = jnp.dot(prepared, wq[...], preferred_element_type=f32)
        k_both = jnp.dot(prepared, wk[...], preferred_element_type=f32)
        v_both = jnp.dot(prepared, wv[...], preferred_element_type=f32)
        factor = HD ** (-0.5)
        for i, slot in enumerate(slots):
            q, k, v = (a[i * rows : (i + 1) * rows] for a in (q_both, k_both, v_both))
            base = pl.multiple_of(WIN + slot * rows, WIN)
            key_value[pl.ds(base, rows), :key_width] = turned(k, slot).astype(bf16)
            key_value[pl.ds(base, rows), key_width:] = v.astype(bf16)
            for h in range(heads):
                lanes = q[:, (h // 2) * 128 : (h // 2 + 1) * 128]
                lanes = (turned(lanes, slot).astype(bf16).astype(f32)) * factor
                at, want = h % 2, h // group
                if at != want:
                    lanes = pltpu.roll(lanes, HD, 1)
                keep = low if want == 0 else jnp.logical_not(low)
                lanes = jnp.where(keep, lanes, 0.0).astype(bf16)
                for n in range(2):
                    queries[2 * slot + n, h * half : (h + 1) * half] = lanes[
                        n * half : (n + 1) * half
                    ]

    loads[8].wait()
    loads[9].wait()

    def fwd(j, c):
        slot = chip_from(j) * 2 + core
        part = pl.ds(c * piece, piece)
        i = (j - 1) * PIECES + c
        return remote(
            rows_all.at[slot, part],
            rows_all.at[slot, part],
            fwd_send.at[i],
            fwd_recv.at[i],
            "tp",
            pair,
        )

    norm_piece(t, 0, rows, 0)
    near.wait_recv()
    norm_piece(pair, 0, rows, rows)
    project((t, pair))
    for j in range(1, chips):
        mine, other = chip_from(j) * 2 + core, chip_from(j) * 2 + 1 - core
        for c in range(PIECES):
            far[j, c].wait_recv()
            fwd(j, c).start()
            norm_piece(mine, c * piece, piece, 0)
            if c:
                fwd(j, c - 1).wait_recv()
                norm_piece(other, (c - 1) * piece, piece, rows)
        fwd(j, PIECES - 1).wait_recv()
        norm_piece(other, (PIECES - 1) * piece, piece, rows)
        project((mine, other))

    halo_right = remote(
        key_value.at[pl.ds(total, WIN)],
        key_value.at[pl.ds(0, WIN)],
        halo_send.at[0],
        halo_recv.at[0],
        "sp",
        lax.rem(s + 1, sp),
    )
    halo_left = remote(
        key_value.at[pl.ds(WIN, WIN)],
        key_value.at[pl.ds(total + WIN, WIN)],
        halo_send.at[1],
        halo_recv.at[1],
        "sp",
        lax.rem(s + sp - 1, sp),
    )
    halo_right.start()
    halo_left.start()
    for copy in ctxs:
        copy.wait()
    loads[10].wait()

    def halves_at(p):
        inner = p < tp - 2
        return (
            jnp.where(inner, p + 2, p - (tp - 2)),
            p + tp,
        )

    def att_pair(b):
        return remote(
            att_all.at[b, t], att_all.at[b, t], apair_send.at[b], apair_recv.at[b], "tp", pair
        )

    def att_far(b, j):
        i = b * (chips - 1) + j - 1
        return remote(
            att_all.at[b, t],
            att_all.at[b, t],
            afar_send.at[i],
            afar_recv.at[i],
            "tp",
            chip_at(j) * 2 + core,
        )

    def att_fwd(b, j):
        slot = chip_from(j) * 2 + core
        i = b * (chips - 1) + j - 1
        return remote(
            att_all.at[b, slot],
            att_all.at[b, slot],
            afwd_send.at[i],
            afwd_recv.at[i],
            "tp",
            pair,
        )

    contract = (((1,), (1,)), ((), ()))
    band = 2 * WIN + half
    stack = heads * half
    q_pos = lax.rem(lax.broadcasted_iota(jnp.int32, (stack, band), 0), half)
    k_pos = lax.broadcasted_iota(jnp.int32, (stack, band), 1)
    in_window = jnp.logical_and(k_pos >= q_pos, k_pos <= q_pos + 2 * WIN)
    head_of = lax.broadcasted_iota(jnp.int32, (stack, 1), 0) // half
    sinks = jnp.full((stack, 1), sink[0], f32)
    for h in range(1, heads):
        sinks = jnp.where(head_of == h, sink[h], sinks)

    def attend(p, n, hb):
        start = pl.multiple_of(hb * half, half)
        band_k = key_value[pl.ds(start, band), :key_width]
        band_v = key_value[pl.ds(start, band), key_width:]
        ctx_k = ctx_kv[:, :, :key_width].reshape(sp * ctx_rows, key_width)
        ctx_v_ = ctx_kv[:, :, key_width:].reshape(sp * ctx_rows, key_width)
        place = s * total + hb * half - WIN + k_pos
        allowed = jnp.logical_and(
            in_window, jnp.logical_and(place >= 0, place < sp * total)
        )
        q = queries[hb]
        near_s = lax.dot_general(q, band_k, contract, preferred_element_type=f32)
        near_s = jnp.where(allowed, near_s, neg_large)
        ctx_s = lax.dot_general(q, ctx_k, contract, preferred_element_type=f32)
        top = jnp.maximum(
            jnp.max(near_s, axis=-1, keepdims=True), jnp.max(ctx_s, axis=-1, keepdims=True)
        )
        top = jnp.maximum(top, sinks)
        near_e = jnp.exp(near_s - top)
        ctx_e = jnp.exp(ctx_s - top)
        bottom = (
            jnp.sum(near_e, axis=-1, keepdims=True)
            + jnp.sum(ctx_e, axis=-1, keepdims=True)
            + jnp.exp(sinks - top)
        )
        share = 1.0 / bottom
        result = jnp.dot(
            (near_e * share).astype(bf16), band_v, preferred_element_type=f32
        ) + jnp.dot((ctx_e * share).astype(bf16), ctx_v_, preferred_element_type=f32)
        for v in range(query_width // 128):
            sides = []
            for at in range(2):
                h = 2 * v + at
                lanes = result[h * half : (h + 1) * half]
                if h // group != at:
                    lanes = pltpu.roll(lanes, HD, 1)
                sides.append(lanes)
            att_all[p, t, n * half : (n + 1) * half, v * 128 : (v + 1) * 128] = jnp.where(
                low[:half], sides[0], sides[1]
            ).astype(bf16)

    def hand_on(b):
        for j in range(1, chips):
            att_far(b, j).wait_recv()
            att_fwd(b, j).start()

    def out_place(hb, source):
        return blended.at[
            pl.ds(pl.multiple_of(lax.rem(hb, 2) * half, half), half),
            pl.ds(pl.multiple_of(source * out_width, 128), out_width),
        ]

    def out_copy(hb):
        return remote(
            out_cols.at[hb],
            out_place(hb, t),
            out_send.at[hb],
            out_recv.at[2 * t + lax.rem(hb, 2)],
            "tp",
            hb // 2,
        )

    def own_copy(hb):
        return pltpu.make_async_copy(
            out_cols.at[hb],
            out_place(hb, t),
            load_sem.at[len(loads) + 1 + lax.rem(hb, 2)],
        )

    def finish(b):
        att_pair(b).wait_recv()
        for j in range(1, chips):
            att_fwd(b, j).wait_recv()
        sums = jnp.dot(att_all[b, 0], wo[0:query_width], preferred_element_type=f32)
        for i in range(1, tp):
            sums = sums + jnp.dot(
                att_all[b, i],
                wo[i * query_width : (i + 1) * query_width],
                preferred_element_type=f32,
            )
        for n, hb in enumerate(halves_at(b)):
            out_cols[hb] = sums[n * half : (n + 1) * half].astype(bf16)

            @pl.when(hb // 2 == t)
            def _():
                own_copy(hb).start()

            @pl.when(hb // 2 != t)
            def _():
                out_copy(hb).start()

    def attend_step(step, carry):
        @pl.when(step < tp)
        def _():
            @pl.when(step == tp - 2)
            def _():
                halo_right.wait_recv()
                halo_left.wait_recv()

            for n, hb in enumerate(halves_at(step)):
                attend(step, n, hb)
            for j in range(1, chips):
                att_far(step, j).start()
            att_pair(step).start()

        @pl.when(jnp.logical_and(step >= 1, step < tp + 1))
        def _():
            hand_on(step - 1)

        @pl.when(step >= 2)
        def _():
            finish(step - 2)

        return carry

    lax.fori_loop(0, tp + 2, attend_step, 0)

    near.wait_send()
    for copy in far.values():
        copy.wait_send()
    for j in range(1, chips):
        for c in range(PIECES):
            fwd(j, c).wait_send()
    gate_store.wait()
    halo_right.wait_send()
    halo_left.wait_send()
    for b in range(tp):
        att_pair(b).wait_send()
        for j in range(1, chips):
            att_far(b, j).wait_send()
            att_fwd(b, j).wait_send()
    for n in range(2):
        own_copy(2 * t + n).wait()
        for k in range(1, tp):
            other = lax.rem(t + k, tp)
            out_copy(2 * other + n).wait_send()
            remote(
                out_cols.at[2 * other + n],
                out_place(2 * t + n, other),
                out_send.at[2 * other + n],
                out_recv.at[2 * other + n],
                "tp",
                other,
            ).wait_recv()


def local(
    latent,
    context,
    conditioning,
    norm_gain,
    shift_weight,
    scale_weight,
    gate_weight,
    query_weight,
    key_weight,
    value_weight,
    out_weight,
    sink_logit,
):
    tp, sp = lax.axis_size("tp"), lax.axis_size("sp")
    rows, width = latent.shape
    ctx_rows = context.shape[0]
    mod_rows, mod_cols = shift_weight.shape
    query_width, key_width = query_weight.shape[1], key_weight.shape[1]
    out_width = out_weight.shape[1]
    fits = (
        rows == WIN
        and key_width == 2 * HD
        and tp % 2 == 0
        and tp >= 4
        and sp >= 2
        and ctx_rows % NORM_ROWS == 0
        and mod_cols % 128 == 0
    )
    if not fits:
        return local_plain(
            latent,
            context,
            conditioning,
            norm_gain,
            shift_weight,
            scale_weight,
            gate_weight,
            query_weight,
            key_weight,
            value_weight,
            out_weight,
            sink_logit,
        )
    f32, bf16 = jnp.float32, jnp.bfloat16
    chips = tp // 2
    far = (chips - 1) * PIECES
    dma = pltpu.SemaphoreType.DMA
    anywhere = pl.BlockSpec(memory_space=pl.ANY)
    blended, gate = pl.pallas_call(
        functools.partial(fused_kernel, tp, sp),
        out_shape=(
            jax.ShapeDtypeStruct((rows, width), bf16),
            jax.ShapeDtypeStruct((1, width), f32),
        ),
        in_specs=[anywhere] * 11 + [pl.BlockSpec(memory_space=pltpu.SMEM)],
        out_specs=(anywhere, anywhere),
        scratch_shapes=[
            pltpu.VMEM((mod_rows,), bf16),
            pltpu.VMEM((1, width), f32),
            pltpu.VMEM((3, mod_rows, mod_cols), bf16),
            pltpu.VMEM(query_weight.shape, bf16),
            pltpu.VMEM(key_weight.shape, bf16),
            pltpu.VMEM(value_weight.shape, bf16),
            pltpu.VMEM(out_weight.shape, bf16),
            pltpu.VMEM(context.shape, bf16),
            pltpu.VMEM((tp, rows, width), bf16),
            pltpu.VMEM((2 * rows, width), bf16),
            pltpu.VMEM((sp, 1, 3 * mod_cols), f32),
            pltpu.VMEM((tp, 1, 3 * mod_cols), f32),
            pltpu.VMEM((1, width), f32),
            pltpu.VMEM((1, width), f32),
            pltpu.VMEM((1, width), f32),
            pltpu.VMEM((tp, rows, 128), f32),
            pltpu.VMEM((tp, rows, 128), f32),
            pltpu.VMEM((2 * tp, query_width // HD * (rows // 2), key_width), bf16),
            pltpu.VMEM(((tp + 2) * rows, 2 * key_width), bf16),
            pltpu.VMEM((sp, ctx_rows, 2 * key_width), bf16),
            pltpu.VMEM((tp, tp, rows, query_width), bf16),
            pltpu.VMEM((2 * tp, rows // 2, out_width), bf16),
            dma((14,)),
            dma((1,)),
            dma((1,)),
            dma((far,)),
            dma((far,)),
            dma((far,)),
            dma((far,)),
            dma((sp - 1,)),
            dma((sp - 1,)),
            dma((tp - 1,)),
            dma((tp - 1,)),
            dma((sp - 1,)),
            dma((sp - 1,)),
            dma((2,)),
            dma((2,)),
            dma((tp,)),
            dma((tp,)),
            dma((tp * (chips - 1),)),
            dma((tp * (chips - 1),)),
            dma((tp * (chips - 1),)),
            dma((tp * (chips - 1),)),
            dma((2 * tp,)),
            dma((2 * tp,)),
        ],
        compiler_params=pltpu.CompilerParams(
            collective_id=0, has_side_effects=True, vmem_limit_bytes=60 * 1024 * 1024
        ),
        name="fused",
    )(
        latent,
        context,
        conditioning,
        norm_gain.reshape(1, width),
        shift_weight,
        scale_weight,
        gate_weight,
        query_weight,
        key_weight,
        value_weight,
        out_weight,
        sink_logit,
    )
    return (latent.astype(f32) + gate * blended.astype(f32)).astype(bf16)


def solution(mesh):
    in_specs = (
        P(("grp", "sp", "tp"), None),
        P(("grp", "sp"), None),
        P(("grp", "sp")),
        P(),
        P("sp", "tp"),
        P("sp", "tp"),
        P("sp", "tp"),
        P(None, "tp"),
        P(None, "tp"),
        P(None, "tp"),
        P(None, "tp"),
        P("tp"),
    )
    out_specs = P(("grp", "sp", "tp"), None)
    return jax.shard_map(local, mesh=mesh, in_specs=in_specs, out_specs=out_specs, check_vma=False)
```
